32 devices in a mesh: ep: 8 (over z, core), tp: 4 (over y, x).
Axes of the slice: x: 2, y: 2, z: 4, core: 2. Of those that a mesh axis runs over, the one named last changes fastest.
Arguments:
- tokens: bfloat16 [512, 2048], P('ep', 'tp'), as said below
- mix_gain: float32 [2048], replicated, may hold values from 0.1 to 1.9
- w_in: bfloat16 [2048, 1024], P(None, 'tp'), may hold values from -0.125 to 0.125
- a_real: float32 [64, 64], P('tp'), may hold values from -1 to -0.1
- a_imag: float32 [64, 64], P('tp'), may hold values from -3.140625 to 3.140625
- log_step: float32 [64], P('tp'), may hold values from -3 to 0
- b_coef: float32 [2, 64, 64, 16], P(None, 'tp'), may hold values from -2.5 to 2.5
- output_coefficients: float32 [2, 64, 16, 64], P(None, 'tp'), may hold values from -1.25 to 1.25
- skip: float32 [1024], P('tp'), may hold values from -6 to 6
- w_out: bfloat16 [1024, 2048], P('tp'), may hold values from -0.1875 to 0.1875
- state: float32 [2, 512, 64, 64], P(None, 'ep', 'tp'), may hold values from -6 to 6
- ffn_gain: float32 [2048], replicated, may hold values from 0.1 to 1.9
- w_gate: bfloat16 [16, 2048, 4096], P('ep', None, 'tp'), may hold values from -0.125 to 0.125
- w_up: bfloat16 [16, 2048, 4096], P('ep', None, 'tp'), may hold values from -0.125 to 0.125
- w_down: bfloat16 [16, 4096, 2048], P('ep', 'tp'), may hold values from -0.09375 to 0.09375
- expert_ids: int32 [512, 2], P('ep'), may hold values from 0 to 15, all different within a row; in each aligned block of 64 rows (0 to 63, 64 to 127, ...) at most 16 rows name the same one
- route_weights: float32 [512, 2], P('ep'), may hold values from 0.3 to 1
Outputs:
- out: bfloat16 [512, 2048], P('ep', 'tp')
- new_state: float32 [2, 512, 64, 64], P(None, 'ep', 'tp')
The draws below stay inside these ranges and needn't reach their ends.
Inputs may be any that keep to these rules, and one draw needn't show every extreme that they name: `expert_ids`: A token's 2 experts differ. Among the 64 rows of one index of ep no expert is named more than 16 times, a bound that some block reaches. `tokens`: feature scales differ along the model width.
All inputs are finite; a program needn't handle non-finite values.
Results may differ from the reference program's by a relative error of at most 0.007.
Values may be sent and summed in bfloat16 or wider, within the bound.
A program may use at most 64 MiB of HBM per device.

```python
import math
import jax
import jax.numpy as jnp
import numpy as np
from jax import lax

D = 2048
S5W = 1024
GROUP_CH = 16
STATE = 64
GROUPS = 64
FFE = 4096
TOPK = 2
EXPERTS = 16
SEQ_DEV = 64
SEQS = 512
CAP = 16
N_EP = 8


def draw_tokens(key, part):
    base_key = jax.random.fold_in(key, 11)
    column = jnp.arange(D, dtype=jnp.float32) / D
    values = jax.random.normal(base_key, (SEQS, D), jnp.float32)
    scaled = values * jnp.exp(column * 1.1)[None, :]
    return scaled.astype(jnp.bfloat16)


def levels(rng, extent, cuts, low, high):
    def one(axis_at, parts):
        steps = jax.random.uniform(jax.random.fold_in(jax.random.fold_in(rng, 6), axis_at), (parts,), jnp.float32, low / len(cuts), high / len(cuts))
        return jnp.repeat(jnp.exp(steps), extent[axis_at] // parts).reshape((-1,) + (1,) * (len(extent) - axis_at - 1))

    loudness = one(*cuts[0])
    for cut in cuts[1:]:
        loudness = loudness * one(*cut)
    return loudness


def assign_block(key, own, number, rows, amount, top, most, lean):
    ranking = jax.random.permutation(key, amount)
    crowded, ordinary = shares(amount, rows * top, most, lean, True), shares(amount, rows * top, most, lean, False)
    places = jnp.arange(amount)

    def named(sizes, rotation):
        used = int((sizes > 0).sum())
        fixed = max(1, used // 4)
        moved = fixed + (places - fixed + rotation * (used - fixed)) % max(1, amount - fixed)
        return jnp.zeros((amount,), jnp.int32).at[ranking[jnp.where(places < fixed, places, moved)]].set(jnp.asarray(sizes, jnp.int32))

    sizes = jnp.where(number % 4 == 0, named(crowded, number // 4), named(ordinary, number - number // 4 - 1))
    mixed = jax.random.permutation(jax.random.fold_in(own, 3), amount)
    donor, receiver = mixed[0:amount // 2 * 2:2], mixed[1:amount // 2 * 2:2]
    room = jnp.minimum(sizes[donor] - 1, most - sizes[receiver]) // 2
    room = jnp.where((donor == ranking[0]) | (receiver == ranking[0]) | (sizes[receiver] == 0), 0, jnp.maximum(room, 0))
    moved = jax.random.randint(jax.random.fold_in(own, 4), (amount // 2,), 0, 1 << 20) % (room + 1)
    sizes = sizes.at[donor].add(-moved).at[receiver].add(moved)
    labels = jnp.searchsorted(jnp.cumsum(sizes), jnp.arange(rows * top), side="right").astype(jnp.int32)
    table = labels.reshape(top, rows).T
    table = table[jax.random.permutation(jax.random.fold_in(own, 1), rows)]
    rotation = jax.random.randint(jax.random.fold_in(own, 2), (rows, 1), 0, top)
    return jnp.take_along_axis(table, (jnp.arange(top)[None, :] + rotation) % top, axis=1)


def shares(number_of, total, reach, skew, full):
    loads = [(1 << 20) // math.isqrt(grade ** skew) + 1 for grade in range(1, number_of + 1)]
    largest = reach if full else min(reach, max(-(-total // number_of), total * loads[0] // sum(loads)))
    least = 1 if total - largest >= number_of - 1 else 0
    given, spare = [largest] + [least] * (number_of - 1), total - largest - least * (number_of - 1)
    while spare > 0:
        movable = [i for i in range(1, number_of) if given[i] < largest] or [i for i in range(1, number_of) if given[i] < reach]
        pool, remaining = sum([loads[i] for i in movable]), spare
        for i in movable:
            more = min(reach - given[i], max(1, remaining * loads[i] // pool), spare)
            given[i] = given[i] + more
            spare = spare - more
    return np.array(given)


def centred(stream_key, shape, spread, bound, cuts=(), held_as=jnp.bfloat16):
    values = spread * jax.random.normal(stream_key, shape, jnp.float32)
    if cuts:
        values = values * levels(stream_key, shape, cuts, -0.22, 0.18)
    return jnp.clip(values, -bound, bound).astype(held_as)


def setup_inputs(seed: int = 0) -> dict:
    keys = jax.random.split(jax.random.key(seed), 18)
    tokens = draw_tokens(jax.random.fold_in(keys[17], 71), 0)
    mix_gain = jnp.clip(1.0 + 0.18 * jax.random.normal(keys[1], (D,), jnp.float32), 0.1, 1.9)
    w_in = centred(keys[2], (D, S5W), D ** -0.5, 0.125, ((1, 4),))
    a_real = jnp.clip(-1.0 + 0.9 * jax.random.uniform(keys[3], (GROUPS, STATE), jnp.float32) ** levels(keys[3], (GROUPS, STATE), ((0, 4),), -0.2, 0.2), -1.0, -0.1)
    a_imag = jnp.clip(jax.random.uniform(keys[4], (GROUPS, STATE), jnp.float32, -3.140625, 3.140625), -3.140625, 3.140625)
    log_step = jnp.clip(-3.0 + 3.0 * jax.random.uniform(keys[5], (GROUPS,), jnp.float32) ** levels(keys[5], (GROUPS,), ((0, 4),), -0.2, 0.2), -3.0, 0.0)
    b_coef = centred(keys[6], (2, GROUPS, STATE, GROUP_CH), ((2 * GROUP_CH) ** -0.5), 2.5, ((1, 4),), jnp.float32)
    output_coefficients = centred(keys[7], (2, GROUPS, GROUP_CH, STATE), ((2 * STATE) ** -0.5), 1.25, ((1, 4),), jnp.float32)
    skip = centred(keys[8], (S5W,), 1.0, 6.0, ((0, 4),), jnp.float32)
    w_out = centred(keys[9], (S5W, D), S5W ** -0.5, 0.1875, ((0, 4),))
    state = centred(keys[10], (2, SEQS, GROUPS, STATE), 1.0, 6.0, ((1, 8), (2, 4)), jnp.float32)
    ffn_gain = jnp.clip(1.0 + 0.18 * jax.random.normal(keys[11], (D,), jnp.float32), 0.1, 1.9)
    w_gate = centred(keys[12], (EXPERTS, D, FFE), D ** -0.5, 0.125, ((0, 8), (2, 4)))
    w_up = centred(keys[13], (EXPERTS, D, FFE), D ** -0.5, 0.125, ((0, 8), (2, 4)))
    w_down = centred(keys[14], (EXPERTS, FFE, D), FFE ** -0.5, 0.09375, ((0, 8), (1, 4)))
    expert_ids_keys = jax.random.split(jax.random.fold_in(keys[15], 1), SEQS // SEQ_DEV)
    expert_ids_turns = jax.random.permutation(jax.random.fold_in(keys[15], 3), SEQS // SEQ_DEV)
    expert_ids = jax.vmap(lambda own, number: assign_block(jax.random.fold_in(keys[15], 2), own, number, SEQ_DEV, EXPERTS, TOPK, CAP, 2))(expert_ids_keys, expert_ids_turns).reshape((SEQS, TOPK))
    route_weights = jnp.clip(0.3 + 0.7 * jax.random.uniform(keys[16], (SEQS, TOPK), jnp.float32) ** levels(keys[16], (SEQS, TOPK), ((0, 8),), -0.2, 0.2), 0.3, 1.0)
    return {"tokens": tokens, "mix_gain": mix_gain, "w_in": w_in, "a_real": a_real, "a_imag": a_imag, "log_step": log_step, "b_coef": b_coef, "output_coefficients": output_coefficients, "skip": skip, "w_out": w_out, "state": state, "ffn_gain": ffn_gain, "w_gate": w_gate, "w_up": w_up, "w_down": w_down, "expert_ids": expert_ids, "route_weights": route_weights}


epsilon = 1e-06
highest_precision = lax.Precision.HIGHEST

def rms_norm(values, gain):
    scaled = values * lax.rsqrt(lax.optimization_barrier(jnp.mean(values * values, axis=-1, keepdims=True)) + epsilon)
    return scaled * gain.astype(jnp.float32)

def state_update(drive, a_real, a_imag, log_step, b_coef, output_coefficients, skip, state):
    count = drive.shape[0]
    groups = a_real.shape[0]
    drive_float = drive.astype(jnp.float32)
    grouped = drive_float.reshape(count, groups, -1)
    step_size = jnp.exp(log_step)[:, None]
    magnitude = jnp.exp(step_size * a_real)
    decay_re = magnitude * jnp.cos(step_size * a_imag)
    decay_imaginary = magnitude * jnp.sin(step_size * a_imag)
    denominator = a_real * a_real + a_imag * a_imag
    shifted = decay_re - 1.0
    factor_re = (shifted * a_real + decay_imaginary * a_imag) / denominator
    factor_im = (decay_imaginary * a_real - shifted * a_imag) / denominator
    coef_re = factor_re[..., None] * b_coef[0] - factor_im[..., None] * b_coef[1]
    coefficient_imaginary = factor_re[..., None] * b_coef[1] + factor_im[..., None] * b_coef[0]
    push_re = jnp.einsum('gpc,sgc->sgp', coef_re, grouped, precision=highest_precision)
    push_im = jnp.einsum('gpc,sgc->sgp', coefficient_imaginary, grouped, precision=highest_precision)
    state_real = decay_re * state[0] - decay_imaginary * state[1] + push_re
    state_imaginary = decay_re * state[1] + decay_imaginary * state[0] + push_im
    state_readout = jnp.einsum('amz,daz->dam', output_coefficients[0], state_real, precision=highest_precision) - jnp.einsum('amz,daz->dam', output_coefficients[1], state_imaginary, precision=highest_precision)
    mixed = state_readout.reshape(count, -1) + skip * drive_float
    return (jax.nn.gelu(mixed).astype(jnp.bfloat16), jnp.stack([state_real, state_imaginary]))

def slot_table(expert_ids, experts, capacity):
    flat_ids = expert_ids.reshape(-1).astype(jnp.int32)
    onehot = (flat_ids[:, None] == jnp.arange(experts, dtype=jnp.int32)[None, :]).astype(jnp.int32)
    ranks = jnp.cumsum(onehot, axis=0) - 1
    slot_rank = lax.optimization_barrier(jnp.sum(onehot * ranks, axis=1))
    slots = flat_ids * capacity + slot_rank
    return (slots[:, None] == jnp.arange(experts * capacity, dtype=jnp.int32)[None, :]).astype(jnp.float32)

def reference(tokens, mix_gain, w_in, a_real, a_imag, log_step, b_coef, output_coefficients, skip, w_out, state, ffn_gain, w_gate, w_up, w_down, expert_ids, route_weights):
    tok_float = tokens.astype(jnp.float32)
    normed = rms_norm(tok_float, mix_gain).astype(jnp.bfloat16)
    drive = jnp.dot(normed, w_in, preferred_element_type=jnp.float32).astype(jnp.bfloat16)
    mixed, new_state = state_update(drive, a_real, a_imag, log_step, b_coef, output_coefficients, skip, state)
    resid = (tok_float + jnp.dot(mixed, w_out, preferred_element_type=jnp.float32)).astype(jnp.bfloat16)
    normed2 = rms_norm(resid.astype(jnp.float32), ffn_gain).astype(jnp.bfloat16)
    placed = jax.vmap(lambda block_ids: slot_table(block_ids, EXPERTS, CAP))(expert_ids.reshape(N_EP, SEQ_DEV, TOPK))
    repeated = jnp.repeat(normed2.reshape(N_EP, SEQ_DEV, D), TOPK, axis=1).astype(jnp.float32)
    buffer = jnp.einsum('nrs,nrd->nsd', placed, repeated, precision=highest_precision).astype(jnp.bfloat16)
    by_expert = buffer.reshape(N_EP, EXPERTS, CAP, D).transpose(1, 0, 2, 3)

    def one_expert(operands):
        slot_rows, gate_weight_matrix, weight_up, weight_down = operands
        flat_rows = slot_rows.reshape(-1, D)
        gate_vals = jnp.dot(flat_rows, gate_weight_matrix, preferred_element_type=jnp.float32)
        up_vals = jnp.dot(flat_rows, weight_up, preferred_element_type=jnp.float32)
        hidden = (jax.nn.silu(gate_vals) * up_vals).astype(jnp.bfloat16)
        result = jnp.dot(hidden, weight_down, preferred_element_type=jnp.float32).astype(jnp.bfloat16)
        return result.reshape(N_EP, CAP, D)
    results = lax.map(one_expert, (by_expert, w_gate, w_up, w_down))
    results = results.transpose(1, 0, 2, 3).reshape(N_EP, EXPERTS * CAP, D).astype(jnp.float32)
    weighted = placed * route_weights.reshape(N_EP, SEQ_DEV * TOPK)[..., None]
    combined = jnp.einsum('nrs,nsd->nrd', weighted, results, precision=highest_precision)
    combined = combined.reshape(SEQS, TOPK, D).sum(axis=1)
    out = (resid.astype(jnp.float32) + combined).astype(jnp.bfloat16)
    return (out, new_state)
```

```python
import functools

import jax
import jax.numpy as jnp
from jax import lax
from jax.experimental import pallas as pl
from jax.experimental.pallas import tpu as pltpu
from jax.sharding import PartitionSpec as P

epsilon = 1e-06
highest_precision = lax.Precision.HIGHEST


def rms_norm(values, gain):
    scaled = values * lax.rsqrt(jnp.mean(values * values, axis=-1, keepdims=True) + epsilon)
    return scaled * gain


def state_update(drive, a_real, a_imag, log_step, b_coef, output_coefficients, skip, state):
    count = drive.shape[0]
    groups = a_real.shape[0]
    drive_float = drive.astype(jnp.float32)
    grouped = drive_float.reshape(count, groups, -1)
    step_size = jnp.exp(log_step)[:, None]
    magnitude = jnp.exp(step_size * a_real)
    decay_re = magnitude * jnp.cos(step_size * a_imag)
    decay_imaginary = magnitude * jnp.sin(step_size * a_imag)
    denominator = a_real * a_real + a_imag * a_imag
    shifted = decay_re - 1.0
    factor_re = (shifted * a_real + decay_imaginary * a_imag) / denominator
    factor_im = (decay_imaginary * a_real - shifted * a_imag) / denominator
    coef_re = factor_re[..., None] * b_coef[0] - factor_im[..., None] * b_coef[1]
    coefficient_imaginary = factor_re[..., None] * b_coef[1] + factor_im[..., None] * b_coef[0]
    push_re = jnp.einsum("gpc,sgc->sgp", coef_re, grouped, precision=highest_precision)
    push_im = jnp.einsum(
        "gpc,sgc->sgp", coefficient_imaginary, grouped, precision=highest_precision
    )
    state_real = decay_re * state[0] - decay_imaginary * state[1] + push_re
    state_imaginary = decay_re * state[1] + decay_imaginary * state[0] + push_im
    state_readout = jnp.einsum(
        "amz,daz->dam", output_coefficients[0], state_real, precision=highest_precision
    ) - jnp.einsum(
        "amz,daz->dam", output_coefficients[1], state_imaginary, precision=highest_precision
    )
    mixed = state_readout.reshape(count, -1) + skip * drive_float
    return (jax.nn.gelu(mixed).astype(jnp.bfloat16), jnp.stack([state_real, state_imaginary]))


def slot_table(expert_ids, experts, capacity):
    flat_ids = expert_ids.reshape(-1)
    onehot = (flat_ids[:, None] == jnp.arange(experts, dtype=jnp.int32)[None, :]).astype(jnp.int32)
    ranks = jnp.cumsum(onehot, axis=0) - 1
    slot_rank = jnp.sum(onehot * ranks, axis=1)
    slots = flat_ids * capacity + slot_rank
    return (slots[:, None] == jnp.arange(experts * capacity, dtype=jnp.int32)[None, :]).astype(
        jnp.float32
    )


def local(
    tokens,
    mix_gain,
    w_in,
    a_real,
    a_imag,
    log_step,
    b_coef,
    output_coefficients,
    skip,
    w_out,
    state,
    ffn_gain,
    w_gate,
    w_up,
    w_down,
    expert_ids,
    route_weights,
):
    seq_count = tokens.shape[0]
    width = tokens.shape[1]
    top_count = expert_ids.shape[1]
    ep_count = lax.axis_size("ep")
    tp_count = lax.axis_size("tp")
    model_width = width * tp_count
    local_experts = w_gate.shape[0]
    experts = local_experts * ep_count
    capacity = max(2, 2 * seq_count * top_count // experts)
    col_start = lax.axis_index("tp") * width
    whole_rows = lax.all_gather(tokens, "tp", axis=1, tiled=True)
    tok_float = whole_rows.astype(jnp.float32)
    normed = rms_norm(tok_float, mix_gain).astype(jnp.bfloat16)
    drive = jnp.dot(normed, w_in, preferred_element_type=jnp.float32).astype(jnp.bfloat16)
    mixed, new_state = state_update(
        drive, a_real, a_imag, log_step, b_coef, output_coefficients, skip, state
    )
    partial_mix = jnp.dot(mixed, w_out, preferred_element_type=jnp.float32)
    placed = slot_table(expert_ids, experts, capacity)
    per_token = (
        placed.reshape(seq_count, top_count, experts * capacity).sum(axis=1).astype(jnp.bfloat16)
    )
    mix_full = lax.psum(partial_mix, "tp")
    resid_full = (tok_float + mix_full).astype(jnp.bfloat16)
    normed2 = rms_norm(resid_full.astype(jnp.float32), ffn_gain).astype(jnp.bfloat16)
    resid_own = lax.dynamic_slice_in_dim(resid_full, col_start, width, 1)
    send_buffer = jnp.dot(per_token.T, normed2, preferred_element_type=jnp.float32).astype(
        jnp.bfloat16
    )
    send_buffer = send_buffer.reshape(ep_count, local_experts, capacity, model_width)
    slot_rows = lax.all_to_all(send_buffer, "ep", split_axis=0, concat_axis=0, tiled=True)
    gate_vals = jnp.einsum("njcd,jdf->njcf", slot_rows, w_gate, preferred_element_type=jnp.float32)
    up_vals = jnp.einsum("njcd,jdf->njcf", slot_rows, w_up, preferred_element_type=jnp.float32)
    hidden = (jax.nn.silu(gate_vals) * up_vals).astype(jnp.bfloat16)
    partial_out = jnp.einsum("njcf,jfd->njcd", hidden, w_down, preferred_element_type=jnp.float32)
    expert_result = lax.psum_scatter(
        partial_out.astype(jnp.bfloat16), "tp", scatter_dimension=3, tiled=True
    )
    returned_rows = lax.all_to_all(expert_result, "ep", split_axis=0, concat_axis=0, tiled=True)
    returned_rows = returned_rows.reshape(experts * capacity, width).astype(jnp.float32)
    weighted = placed * route_weights.reshape(-1)[:, None]
    combined = jnp.dot(weighted, returned_rows, precision=highest_precision)
    combined = combined.reshape(seq_count, top_count, width).sum(axis=1)
    out = (resid_own.astype(jnp.float32) + combined).astype(jnp.bfloat16)
    return (out, new_state)


MESH = pl.DeviceIdType.MESH
HBM = pltpu.HBM


def log2(value):
    return value.bit_length() - 1


def iota(shape, axis):
    return lax.broadcasted_iota(jnp.int32, shape, axis)


def nt_dot(left, right):
    return lax.dot_general(
        left, right, (((1,), (1,)), ((), ())), preferred_element_type=jnp.float32
    )


def nn_dot(left, right):
    return jnp.dot(left, right, preferred_element_type=jnp.float32)


def fused_body(
    sizes,
    tokens, mix_gain, w_in, a_real, a_imag, log_step, b_coef, out_coef, skip, w_out, state,
    ffn_gain, w_gate, w_up, w_down, ids, route,
    out, new_state,
    tok_v, mg_v, win_v, ar_v, ai_v, ls_v, b_v, oc_v, skip_v, wo_v, st_v, fg_v, wg_v, wu_v, wd_v,
    ids_v, rw_v,
    bt_v, ct_v, rows_v, base_v, ns_v, half_v, part_v, part_in, sel_v, pick_v, resid_v, slot_v,
    x_v, xn_v, hid_v, oo_v, own_v, oo_in, ro_v, ret_v, out_v,
    load_sem, wload_sem, store_sem,
    ag_s, ag_r, rs_s, rs_r, dp_s, dp_r, fw_s, fw_r, os_s, os_r, rt_s, rt_r,
):
    n_tp, n_ep, seqs, width, groups, states, chans, cap, local_e, hidden = sizes
    bf16, f32 = jnp.bfloat16, jnp.float32
    model = width * n_tp
    lanes = groups * states
    channels = groups * chans
    slots = cap * local_e
    me_t = lax.axis_index("tp")
    me_e = lax.axis_index("ep")

    def tp_to(d):
        return lax.rem(me_t + d, n_tp)

    def ep_to(d):
        return lax.rem(me_e + d, n_ep)

    def ep_from(d):
        return lax.rem(me_e + n_ep - d, n_ep)

    def remote(src, dst, send, recv, device):
        return pltpu.make_async_remote_copy(
            src_ref=src, dst_ref=dst, send_sem=send, recv_sem=recv,
            device_id=device, device_id_type=MESH,
        )

    loads = {}

    def load(name, src, dst, sem):
        copy = pltpu.make_async_copy(src, dst, sem)
        copy.start()
        loads[name] = copy

    load("tok", tokens, tok_v.at[me_t], load_sem.at[0])
    small = (
        ("ar", a_real, ar_v), ("ai", a_imag, ai_v), ("ls", log_step, ls_v), ("b", b_coef, b_v),
        ("oc", out_coef, oc_v), ("st", state, st_v), ("mg", mix_gain, mg_v), ("win", w_in, win_v),
        ("skip", skip, skip_v), ("wo", w_out, wo_v), ("ids", ids, ids_v), ("rw", route, rw_v),
        ("fg", ffn_gain, fg_v),
    )
    for at, (name, src, dst) in enumerate(small):
        load(name, src, dst, load_sem.at[at + 1])

    barrier = pltpu.get_barrier_semaphore()
    for d in range(1, n_tp):
        pl.semaphore_signal(barrier, inc=1, device_id={"tp": tp_to(d)}, device_id_type=MESH)
    for d in range(1, n_ep):
        pl.semaphore_signal(barrier, inc=1, device_id={"ep": ep_to(d)}, device_id_type=MESH)
    loads["tok"].wait()
    pl.semaphore_wait(barrier, n_tp + n_ep - 2)

    gathers = []
    for d in range(1, n_tp):
        copy = remote(
            tok_v.at[me_t], tok_v.at[me_t], ag_s.at[d - 1], ag_r.at[d - 1], {"tp": tp_to(d)}
        )
        copy.start()
        gathers.append(copy)
    for j in range(local_e):
        load(("g", j), w_gate.at[j], wg_v.at[j], wload_sem.at[3 * j])
        load(("u", j), w_up.at[j], wu_v.at[j], wload_sem.at[3 * j + 1])
        load(("d", j), w_down.at[j], wd_v.at[j], wload_sem.at[3 * j + 2])

    for name in ("ar", "ai", "ls"):
        loads[name].wait()
    log_col = jnp.sum(
        jnp.where(iota((groups, groups), 0) == iota((groups, groups), 1), ls_v[...], 0.0),
        axis=1, keepdims=True,
    )
    step_size = jnp.exp(log_col)
    re, im = ar_v[...], ai_v[...]
    magnitude = jnp.exp(step_size * re)
    decay_re = magnitude * jnp.cos(step_size * im)
    decay_im = magnitude * jnp.sin(step_size * im)
    denominator = re * re + im * im
    shifted = decay_re - 1.0
    factor_re = (shifted * re + decay_im * im) / denominator
    factor_im = (decay_im * re - shifted * im) / denominator
    spread_state = (
        jnp.bitwise_and(iota((states, lanes), 1), states - 1) == iota((states, lanes), 0)
    )
    own_group = jnp.right_shift(iota((groups, lanes), 1), log2(states)) == iota((groups, lanes), 0)
    spread_f32 = spread_state.astype(f32)
    for at, value in enumerate((decay_re, decay_im, factor_re, factor_im)):
        wide = jnp.dot(
            value, spread_f32, precision=highest_precision, preferred_element_type=f32
        )
        rows_v[pl.ds(at, 1), :] = jnp.sum(jnp.where(own_group, wide, 0.0), axis=0, keepdims=True)

    loads["b"].wait()
    spread_chan = (
        jnp.bitwise_and(iota((chans, channels), 1), chans - 1) == iota((chans, channels), 0)
    ).astype(bf16)
    b_mask = jnp.right_shift(iota((lanes, channels), 0), log2(states)) == jnp.right_shift(
        iota((lanes, channels), 1), log2(chans)
    )
    for i in range(2):
        bt_v[i] = jnp.where(b_mask, nn_dot(b_v[i].astype(bf16), spread_chan), 0.0).astype(bf16)
    loads["oc"].wait()
    c_mask = jnp.right_shift(iota((channels, lanes), 0), log2(chans)) == jnp.right_shift(
        iota((channels, lanes), 1), log2(states)
    )
    for i in range(2):
        ct_v[i] = jnp.where(
            c_mask, nn_dot(oc_v[i].astype(bf16), spread_state.astype(bf16)), 0.0
        ).astype(bf16)

    loads["st"].wait()
    pairs = 128 // states
    for piece in range(groups // pairs):
        at = pl.ds(piece * 128, 128)
        old = []
        for i in range(2):
            old.append(
                jnp.concatenate(
                    [
                        st_v[i, pl.ds(piece * pairs + k, seqs, stride=groups), :]
                        for k in range(pairs)
                    ],
                    axis=1,
                )
            )
        d_re, d_im = rows_v[pl.ds(0, 1), at], rows_v[pl.ds(1, 1), at]
        base_v[0, :, at] = d_re * old[0] - d_im * old[1]
        base_v[1, :, at] = d_re * old[1] + d_im * old[0]

    loads["ids"].wait()
    experts = n_ep * local_e
    all_slots = experts * cap
    chosen = [
        (ids_v[:, k : k + 1] == iota((seqs, experts), 1)).astype(bf16)
        for k in range(ids_v.shape[1])
    ]
    named = chosen[0]
    for one in chosen[1:]:
        named = named + one
    earlier = (iota((seqs, seqs), 1) < iota((seqs, seqs), 0)).astype(bf16)
    rank = nn_dot(earlier, named).astype(bf16)
    tall = (
        jnp.right_shift(iota((all_slots, experts), 0), log2(cap)) == iota((all_slots, experts), 1)
    ).astype(bf16)
    tall_rank = jnp.bitwise_and(iota((all_slots, seqs), 0), cap - 1).astype(f32)
    hit = (nt_dot(tall, named) > 0.5) & (nt_dot(tall, rank) == tall_rank)
    sel_v[...] = hit.astype(f32).astype(bf16)
    wide_rank = jnp.bitwise_and(iota((seqs, all_slots), 1), cap - 1).astype(f32)
    right_rank = nt_dot(rank, tall) == wide_rank
    for k, one in enumerate(chosen):
        pick_v[k] = ((nt_dot(one, tall) > 0.5) & right_rank).astype(f32).astype(bf16)

    loads["mg"].wait()
    loads["win"].wait()
    for copy in gathers:
        copy.wait_recv()
    square = jnp.zeros((seqs, 1), f32)
    for t in range(n_tp):
        value = tok_v[t].astype(f32)
        square = square + jnp.sum(value * value, axis=1, keepdims=True)
    scale = lax.rsqrt(square * (1.0 / model) + epsilon)
    drive = jnp.zeros((seqs, channels), f32)
    for t in range(n_tp):
        columns = pl.ds(t * width, width)
        normed = (tok_v[t].astype(f32) * scale * mg_v[:, columns]).astype(bf16)
        drive = drive + nn_dot(normed, win_v[columns, :])
    drive = drive.astype(bf16)
    push = [nt_dot(drive, bt_v[i]) for i in range(2)]
    for piece in range(groups // pairs):
        lo = piece * 128
        at = pl.ds(lo, 128)
        f_re, f_im = rows_v[pl.ds(2, 1), at], rows_v[pl.ds(3, 1), at]
        x_re, x_im = push[0][:, lo : lo + 128], push[1][:, lo : lo + 128]
        new = (
            base_v[0, :, at] + (f_re * x_re - f_im * x_im),
            base_v[1, :, at] + (f_re * x_im + f_im * x_re),
        )
        for i in range(2):
            half_v[i, :, at] = new[i].astype(bf16)
            base_v[i, :, at] = new[i]
    readout = nt_dot(half_v[0], ct_v[0]) - nt_dot(half_v[1], ct_v[1])
    loads["skip"].wait()
    mixed = jax.nn.gelu(readout + skip_v[...] * drive.astype(f32)).astype(bf16)

    loads["wo"].wait()
    scatters = []
    for d in range(1, n_tp):
        columns = pl.ds(pl.multiple_of(tp_to(d) * width, 128), width)
        part_v[d - 1] = nn_dot(mixed, wo_v[:, columns]).astype(bf16)
        copy = remote(
            part_v.at[d - 1], part_in.at[d - 1], rs_s.at[d - 1], rs_r.at[d - 1], {"tp": tp_to(d)}
        )
        copy.start()
        scatters.append(copy)
    columns = pl.ds(pl.multiple_of(me_t * width, 128), width)
    total = nn_dot(mixed, wo_v[:, columns]) + tok_v[me_t].astype(f32)
    for piece in range(groups // pairs):
        for i in range(2):
            for k in range(pairs):
                ns_v[i, pl.ds(piece * pairs + k, seqs, stride=groups), :] = base_v[
                    i, :, piece * 128 + k * states : piece * 128 + (k + 1) * states
                ]
    keep_state = pltpu.make_async_copy(ns_v, new_state, store_sem.at[0])
    keep_state.start()
    for d in range(1, n_tp):
        scatters[d - 1].wait_recv()
        total = total + part_in[d - 1].astype(f32)
    resid = total.astype(bf16)
    resid_v[...] = resid

    slot_rows = nn_dot(sel_v[...], resid).astype(bf16)
    slot_v[...] = slot_rows.reshape(n_ep, slots, width)
    dispatches = {}
    for d in range(1, n_ep):
        copy = remote(
            slot_v.at[ep_to(d)], x_v.at[me_t, me_e], dp_s.at[d - 1], dp_r.at[d - 1],
            {"ep": ep_to(d)},
        )
        copy.start()
        dispatches[d] = copy
    x_v[me_t, me_e] = slot_v[me_e]
    forwards = []
    for d in range(n_ep):
        if d:
            dispatches[d].wait_recv()
        block = x_v.at[me_t, ep_from(d)]
        for k in range(1, n_tp):
            sem = d * (n_tp - 1) + k - 1
            copy = remote(block, block, fw_s.at[sem], fw_r.at[sem], {"tp": tp_to(k)})
            copy.start()
            forwards.append(copy)
    for copy in forwards:
        copy.wait_recv()

    loads["fg"].wait()
    rows = n_ep * cap
    out_copies = []
    for j in range(local_e):
        blocks = [x_v[t, :, pl.ds(j * cap, cap), :].reshape(rows, width) for t in range(n_tp)]
        square = jnp.zeros((rows, 1), f32)
        for value in blocks:
            value = value.astype(f32)
            square = square + jnp.sum(value * value, axis=1, keepdims=True)
        scale = lax.rsqrt(square * (1.0 / model) + epsilon)
        for t in range(n_tp):
            columns = pl.ds(t * width, width)
            xn_v[:, columns] = (blocks[t].astype(f32) * scale * fg_v[:, columns]).astype(bf16)
        loads[("g", j)].wait()
        loads[("u", j)].wait()
        tile = 256

        @pl.loop(0, hidden // tile)
        def _(n, j=j):
            at = pl.ds(pl.multiple_of(n * tile, tile), tile)
            gate = nn_dot(xn_v[...], wg_v[j, :, at])
            up = nn_dot(xn_v[...], wu_v[j, :, at])
            hid_v[:, at] = (jax.nn.silu(gate) * up).astype(bf16)

        loads[("d", j)].wait()
        for d in range(1, n_tp):
            columns = pl.ds(pl.multiple_of(tp_to(d) * width, 128), width)
            at = j * (n_tp - 1) + d - 1
            oo_v[at] = nn_dot(hid_v[...], wd_v[j, :, columns]).astype(bf16)
            copy = remote(oo_v.at[at], oo_in.at[at], os_s.at[at], os_r.at[at], {"tp": tp_to(d)})
            copy.start()
            out_copies.append(copy)
        columns = pl.ds(pl.multiple_of(me_t * width, 128), width)
        own_v[j] = nn_dot(hid_v[...], wd_v[j, :, columns])

    returns = []
    for j in range(local_e):
        total = own_v[j]
        for d in range(1, n_tp):
            at = j * (n_tp - 1) + d - 1
            out_copies[at].wait_recv()
            total = total + oo_in[at].astype(f32)
        ro_v[j] = total.astype(bf16).reshape(n_ep, cap, width)
        for d in range(1, n_ep):
            at = j * (n_ep - 1) + d - 1
            copy = remote(
                ro_v.at[j, ep_to(d)], ret_v.at[me_e, j], rt_s.at[at], rt_r.at[at],
                {"ep": ep_to(d)},
            )
            copy.start()
            returns.append(copy)
        ret_v[me_e, j] = ro_v[j, me_e]
    loads["rw"].wait()
    for copy in returns:
        copy.wait_recv()
    result = resid_v[...].astype(f32)
    back = ret_v[...].reshape(all_slots, width)
    for k in range(len(chosen)):
        result = result + rw_v[:, k : k + 1] * nn_dot(pick_v[k], back)
    out_v[...] = result.astype(bf16)
    keep_out = pltpu.make_async_copy(out_v, out, store_sem.at[1])
    keep_out.start()
    for copy in gathers + scatters + list(dispatches.values()) + forwards + out_copies + returns:
        copy.wait_send()
    keep_state.wait()
    keep_out.wait()


def fused(
    tokens, mix_gain, w_in, a_real, a_imag, log_step, b_coef, output_coefficients, skip, w_out,
    state, ffn_gain, w_gate, w_up, w_down, expert_ids, route_weights,
):
    bf16, f32 = jnp.bfloat16, jnp.float32
    n_tp, n_ep = lax.axis_size("tp"), lax.axis_size("ep")
    seqs, width = tokens.shape
    groups, states = a_real.shape
    chans = b_coef.shape[3]
    local_e, model, hidden = w_gate.shape
    top = expert_ids.shape[1]
    experts = local_e * n_ep
    cap = max(2, 2 * seqs * top // experts)
    lanes, channels = groups * states, groups * chans
    slots, rows = cap * local_e, n_ep * cap
    sizes = (n_tp, n_ep, seqs, width, groups, states, chans, cap, local_e, hidden)
    args = (
        tokens, mix_gain[None], w_in, a_real, a_imag, log_step[None],
        b_coef.reshape(2, lanes, chans), output_coefficients.reshape(2, channels, states),
        skip[None], w_out, state.reshape(2, seqs * groups, states), ffn_gain[None],
        w_gate, w_up, w_down, expert_ids, route_weights,
    )
    vmem = pltpu.VMEM
    scratch = [vmem((n_tp, seqs, width), bf16)]
    scratch += [vmem(a.shape, a.dtype) for a in args[1:]]
    scratch += [
        vmem((2, lanes, channels), bf16),
        vmem((2, channels, lanes), bf16),
        vmem((8, lanes), f32),
        vmem((2, seqs, lanes), f32),
        vmem((2, seqs * groups, states), f32),
        vmem((2, seqs, lanes), bf16),
        vmem((n_tp - 1, seqs, width), bf16),
        vmem((n_tp - 1, seqs, width), bf16),
        vmem((experts * cap, seqs), bf16),
        vmem((top, seqs, experts * cap), bf16),
        vmem((seqs, width), bf16),
        vmem((n_ep, slots, width), bf16),
        vmem((n_tp, n_ep, slots, width), bf16),
        vmem((rows, model), bf16),
        vmem((rows, hidden), bf16),
        vmem((local_e * (n_tp - 1), rows, width), bf16),
        vmem((local_e, rows, width), f32),
        vmem((local_e * (n_tp - 1), rows, width), bf16),
        vmem((local_e, n_ep, cap, width), bf16),
        vmem((n_ep, local_e, cap, width), bf16),
        vmem((seqs, width), bf16),
    ]
    dma = pltpu.SemaphoreType.DMA
    counts = [14, 3 * local_e, 2]
    for number in (
        n_tp - 1, n_tp - 1, n_ep - 1, n_ep * (n_tp - 1), local_e * (n_tp - 1), local_e * (n_ep - 1)
    ):
        counts += [number, number]
    scratch += [dma((number,)) for number in counts]
    out, new_state = pl.pallas_call(
        functools.partial(fused_body, sizes),
        out_shape=(
            jax.ShapeDtypeStruct((seqs, width), bf16),
            jax.ShapeDtypeStruct((2, seqs * groups, states), f32),
        ),
        in_specs=[pl.BlockSpec(memory_space=HBM)] * len(args),
        out_specs=(pl.BlockSpec(memory_space=HBM),) * 2,
        scratch_shapes=scratch,
        compiler_params=pltpu.CompilerParams(
            collective_id=0, has_side_effects=True, vmem_limit_bytes=60 * 1024 * 1024
        ),
    )(*args)
    return out, new_state.reshape(state.shape)


def fits(mesh_tp, width, groups, states, chans, cap, hidden):
    powers = all(v & (v - 1) == 0 for v in (states, chans, cap))
    return (
        powers and width % 128 == 0 and states <= 128 and groups % max(8, 128 // states) == 0
        and cap % 16 == 0 and (groups * chans) % 128 == 0 and hidden % 256 == 0
    )


def layer(*args):
    tokens, a_real, b_coef, w_gate, ids = args[0], args[3], args[6], args[12], args[15]
    experts = w_gate.shape[0] * lax.axis_size("ep")
    cap = max(2, 2 * tokens.shape[0] * ids.shape[1] // experts)
    kernel = fits(
        lax.axis_size("tp"), tokens.shape[1], *a_real.shape, b_coef.shape[3], cap, w_gate.shape[2]
    )
    return fused(*args) if kernel else local(*args)


def solution(mesh):
    in_specs = (
        P("ep", "tp"),
        P(),
        P(None, "tp"),
        P("tp", None),
        P("tp", None),
        P("tp"),
        P(None, "tp", None, None),
        P(None, "tp", None, None),
        P("tp"),
        P("tp", None),
        P(None, "ep", "tp", None),
        P(),
        P("ep", None, "tp"),
        P("ep", None, "tp"),
        P("ep", "tp", None),
        P("ep", None),
        P("ep", None),
    )
    out_specs = (P("ep", "tp"), P(None, "ep", "tp", None))
    return jax.shard_map(layer, mesh=mesh, in_specs=in_specs, out_specs=out_specs, check_vma=False)
```

```python
import functools

import jax
import jax.numpy as jnp
from jax import lax
from jax.experimental import pallas as pl
from jax.experimental.pallas import tpu as pltpu
from jax.sharding import PartitionSpec as P

epsilon = 1e-06
highest_precision = lax.Precision.HIGHEST


def rms_norm(values, gain):
    scaled = values * lax.rsqrt(jnp.mean(values * values, axis=-1, keepdims=True) + epsilon)
    return scaled * gain


def state_update(drive, a_real, a_imag, log_step, b_coef, output_coefficients, skip, state):
    count = drive.shape[0]
    groups = a_real.shape[0]
    drive_float = drive.astype(jnp.float32)
    grouped = drive_float.reshape(count, groups, -1)
    step_size = jnp.exp(log_step)[:, None]
    magnitude = jnp.exp(step_size * a_real)
    decay_re = magnitude * jnp.cos(step_size * a_imag)
    decay_imaginary = magnitude * jnp.sin(step_size * a_imag)
    denominator = a_real * a_real + a_imag * a_imag
    shifted = decay_re - 1.0
    factor_re = (shifted * a_real + decay_imaginary * a_imag) / denominator
    factor_im = (decay_imaginary * a_real - shifted * a_imag) / denominator
    coef_re = factor_re[..., None] * b_coef[0] - factor_im[..., None] * b_coef[1]
    coefficient_imaginary = factor_re[..., None] * b_coef[1] + factor_im[..., None] * b_coef[0]
    push_re = jnp.einsum("gpc,sgc->sgp", coef_re, grouped, precision=highest_precision)
    push_im = jnp.einsum(
        "gpc,sgc->sgp", coefficient_imaginary, grouped, precision=highest_precision
    )
    state_real = decay_re * state[0] - decay_imaginary * state[1] + push_re
    state_imaginary = decay_re * state[1] + decay_imaginary * state[0] + push_im
    state_readout = jnp.einsum(
        "amz,daz->dam", output_coefficients[0], state_real, precision=highest_precision
    ) - jnp.einsum(
        "amz,daz->dam", output_coefficients[1], state_imaginary, precision=highest_precision
    )
    mixed = state_readout.reshape(count, -1) + skip * drive_float
    return (jax.nn.gelu(mixed).astype(jnp.bfloat16), jnp.stack([state_real, state_imaginary]))


def slot_table(expert_ids, experts, capacity):
    flat_ids = expert_ids.reshape(-1)
    onehot = (flat_ids[:, None] == jnp.arange(experts, dtype=jnp.int32)[None, :]).astype(jnp.int32)
    ranks = jnp.cumsum(onehot, axis=0) - 1
    slot_rank = jnp.sum(onehot * ranks, axis=1)
    slots = flat_ids * capacity + slot_rank
    return (slots[:, None] == jnp.arange(experts * capacity, dtype=jnp.int32)[None, :]).astype(
        jnp.float32
    )


def local(
    tokens,
    mix_gain,
    w_in,
    a_real,
    a_imag,
    log_step,
    b_coef,
    output_coefficients,
    skip,
    w_out,
    state,
    ffn_gain,
    w_gate,
    w_up,
    w_down,
    expert_ids,
    route_weights,
):
    seq_count = tokens.shape[0]
    width = tokens.shape[1]
    top_count = expert_ids.shape[1]
    ep_count = lax.axis_size("ep")
    tp_count = lax.axis_size("tp")
    model_width = width * tp_count
    local_experts = w_gate.shape[0]
    experts = local_experts * ep_count
    capacity = max(2, 2 * seq_count * top_count // experts)
    col_start = lax.axis_index("tp") * width
    whole_rows = lax.all_gather(tokens, "tp", axis=1, tiled=True)
    tok_float = whole_rows.astype(jnp.float32)
    normed = rms_norm(tok_float, mix_gain).astype(jnp.bfloat16)
    drive = jnp.dot(normed, w_in, preferred_element_type=jnp.float32).astype(jnp.bfloat16)
    mixed, new_state = state_update(
        drive, a_real, a_imag, log_step, b_coef, output_coefficients, skip, state
    )
    partial_mix = jnp.dot(mixed, w_out, preferred_element_type=jnp.float32)
    placed = slot_table(expert_ids, experts, capacity)
    per_token = (
        placed.reshape(seq_count, top_count, experts * capacity).sum(axis=1).astype(jnp.bfloat16)
    )
    mix_full = lax.psum(partial_mix, "tp")
    resid_full = (tok_float + mix_full).astype(jnp.bfloat16)
    normed2 = rms_norm(resid_full.astype(jnp.float32), ffn_gain).astype(jnp.bfloat16)
    resid_own = lax.dynamic_slice_in_dim(resid_full, col_start, width, 1)
    send_buffer = jnp.dot(per_token.T, normed2, preferred_element_type=jnp.float32).astype(
        jnp.bfloat16
    )
    send_buffer = send_buffer.reshape(ep_count, local_experts, capacity, model_width)
    slot_rows = lax.all_to_all(send_buffer, "ep", split_axis=0, concat_axis=0, tiled=True)
    gate_vals = jnp.einsum("njcd,jdf->njcf", slot_rows, w_gate, preferred_element_type=jnp.float32)
    up_vals = jnp.einsum("njcd,jdf->njcf", slot_rows, w_up, preferred_element_type=jnp.float32)
    hidden = (jax.nn.silu(gate_vals) * up_vals).astype(jnp.bfloat16)
    partial_out = jnp.einsum("njcf,jfd->njcd", hidden, w_down, preferred_element_type=jnp.float32)
    expert_result = lax.psum_scatter(
        partial_out.astype(jnp.bfloat16), "tp", scatter_dimension=3, tiled=True
    )
    returned_rows = lax.all_to_all(expert_result, "ep", split_axis=0, concat_axis=0, tiled=True)
    returned_rows = returned_rows.reshape(experts * capacity, width).astype(jnp.float32)
    weighted = placed * route_weights.reshape(-1)[:, None]
    combined = jnp.dot(weighted, returned_rows, precision=highest_precision)
    combined = combined.reshape(seq_count, top_count, width).sum(axis=1)
    out = (resid_own.astype(jnp.float32) + combined).astype(jnp.bfloat16)
    return (out, new_state)


MESH = pl.DeviceIdType.MESH
HBM = pltpu.HBM


def log2(value):
    return value.bit_length() - 1


def iota(shape, axis):
    return lax.broadcasted_iota(jnp.int32, shape, axis)


def nt_dot(left, right):
    return lax.dot_general(
        left, right, (((1,), (1,)), ((), ())), preferred_element_type=jnp.float32
    )


def nn_dot(left, right):
    return jnp.dot(left, right, preferred_element_type=jnp.float32)


def to_column(row):
    shape = (row.shape[1], row.shape[1])
    return jnp.sum(jnp.where(iota(shape, 0) == iota(shape, 1), row, 0.0), axis=1, keepdims=True)


def fused_body(
    sizes,
    tokens, mix_gain, w_in, a_real, a_imag, log_step, b_coef, out_coef, skip, w_out, state,
    ffn_gain, w_gate, w_up, w_down, ids, route,
    out, new_state,
    tok_v, mg_v, win_v, ar_v, ai_v, ls_v, b_v, oc_v, skip_v, wo_v, st_v, fg_v, wg_v, wu_v, wd_v,
    ids_v, rw_v,
    bt_v, ct_v, rows_v, base_v, ns_v, half_v, part_v, part_in, sel_v, pick_v, resid_v, slot_v,
    x_v, xn_v, hid_v, oo_v, own_v, oo_in, ro_v, ret_v, out_v,
    load_sem, wload_sem, store_sem,
    ag_s, ag_r, rs_s, rs_r, dp_s, dp_r, fw_s, fw_r, os_s, os_r, rt_s, rt_r,
):
    n_tp, n_ep, seqs, width, groups, states, chans, cap, local_e, hidden = sizes
    bf16, f32 = jnp.bfloat16, jnp.float32
    model = width * n_tp
    lanes = groups * states
    channels = groups * chans
    me_t = lax.axis_index("tp")
    me_e = lax.axis_index("ep")

    def tp_to(d):
        return lax.rem(me_t + d, n_tp)

    def ep_to(d):
        return lax.rem(me_e + d, n_ep)

    def ep_from(d):
        return lax.rem(me_e + n_ep - d, n_ep)

    def remote(src, dst, send, recv, device):
        return pltpu.make_async_remote_copy(
            src_ref=src, dst_ref=dst, send_sem=send, recv_sem=recv,
            device_id=device, device_id_type=MESH,
        )

    loads = {}

    def load(name, src, dst, sem):
        copy = pltpu.make_async_copy(src, dst, sem)
        copy.start()
        loads[name] = copy

    load("tok", tokens, tok_v.at[me_t], load_sem.at[0])
    small = (
        ("ar", a_real, ar_v), ("ai", a_imag, ai_v), ("ls", log_step, ls_v), ("b", b_coef, b_v),
        ("oc", out_coef, oc_v), ("st", state, st_v), ("mg", mix_gain, mg_v), ("win", w_in, win_v),
        ("skip", skip, skip_v), ("wo", w_out, wo_v), ("ids", ids, ids_v), ("rw", route, rw_v),
        ("fg", ffn_gain, fg_v),
    )
    for at, (name, src, dst) in enumerate(small):
        load(name, src, dst, load_sem.at[at + 1])

    barrier = pltpu.get_barrier_semaphore()
    for d in range(1, n_tp):
        pl.semaphore_signal(barrier, inc=1, device_id={"tp": tp_to(d)}, device_id_type=MESH)
    for d in range(1, n_ep):
        pl.semaphore_signal(barrier, inc=1, device_id={"ep": ep_to(d)}, device_id_type=MESH)
    loads["tok"].wait()
    pl.semaphore_wait(barrier, n_tp + n_ep - 2)

    gathers = []
    for d in range(1, n_tp):
        copy = remote(
            tok_v.at[me_t], tok_v.at[me_t], ag_s.at[d - 1], ag_r.at[d - 1], {"tp": tp_to(d)}
        )
        copy.start()
        gathers.append(copy)
    for j in range(local_e):
        load(("g", j), w_gate.at[j], wg_v.at[j], wload_sem.at[3 * j])
        load(("u", j), w_up.at[j], wu_v.at[j], wload_sem.at[3 * j + 1])
        load(("d", j), w_down.at[j], wd_v.at[j], wload_sem.at[3 * j + 2])

    for name in ("ar", "ai", "ls"):
        loads[name].wait()
    step_size = jnp.exp(to_column(ls_v[...]))
    re, im = ar_v[...], ai_v[...]
    magnitude = jnp.exp(step_size * re)
    decay_re = magnitude * jnp.cos(step_size * im)
    decay_im = magnitude * jnp.sin(step_size * im)
    denominator = re * re + im * im
    shifted = decay_re - 1.0
    factor_re = (shifted * re + decay_im * im) / denominator
    factor_im = (decay_im * re - shifted * im) / denominator
    spread_state = (
        jnp.bitwise_and(iota((states, lanes), 1), states - 1) == iota((states, lanes), 0)
    )
    own_group = jnp.right_shift(iota((groups, lanes), 1), log2(states)) == iota((groups, lanes), 0)
    spread_f32 = spread_state.astype(f32)
    for at, value in enumerate((decay_re, decay_im, factor_re, factor_im)):
        wide = jnp.dot(
            value, spread_f32, precision=highest_precision, preferred_element_type=f32
        )
        rows_v[pl.ds(at, 1), :] = jnp.sum(jnp.where(own_group, wide, 0.0), axis=0, keepdims=True)

    block = jnp.right_shift(iota((channels, lanes), 0), log2(chans)) == jnp.right_shift(
        iota((channels, lanes), 1), log2(states)
    )
    spread_bf16 = spread_f32.astype(bf16)
    for name, src, dst in (("b", b_v, bt_v), ("oc", oc_v, ct_v)):
        loads[name].wait()
        for i in range(2):
            dst[i] = jnp.where(block, nn_dot(src[i].astype(bf16), spread_bf16), 0.0).astype(bf16)

    loads["st"].wait()
    pairs = 128 // states
    for piece in range(groups // pairs):
        at = pl.ds(piece * 128, 128)
        old = []
        for i in range(2):
            old.append(
                jnp.concatenate(
                    [
                        st_v[i, pl.ds(piece * pairs + k, seqs, stride=groups), :]
                        for k in range(pairs)
                    ],
                    axis=1,
                )
            )
        d_re, d_im = rows_v[pl.ds(0, 1), at], rows_v[pl.ds(1, 1), at]
        base_v[0, :, at] = d_re * old[0] - d_im * old[1]
        base_v[1, :, at] = d_re * old[1] + d_im * old[0]

    loads["ids"].wait()
    experts = n_ep * local_e
    all_slots = experts * cap
    chosen = [
        (
            to_column(ids_v[k : k + 1, :].astype(f32)) == iota((seqs, experts), 1).astype(f32)
        ).astype(bf16)
        for k in range(ids_v.shape[0])
    ]
    named = chosen[0]
    for one in chosen[1:]:
        named = named + one
    earlier = (iota((seqs, seqs), 1) < iota((seqs, seqs), 0)).astype(bf16)
    rank = nn_dot(earlier, named).astype(bf16)
    tall = (
        jnp.right_shift(iota((all_slots, experts), 0), log2(cap)) == iota((all_slots, experts), 1)
    ).astype(bf16)
    tall_rank = jnp.bitwise_and(iota((all_slots, seqs), 0), cap - 1).astype(f32)
    hit = (nt_dot(tall, named) > 0.5) & (nt_dot(tall, rank) == tall_rank)
    sel_v[...] = hit.astype(f32).astype(bf16)
    wide_rank = jnp.bitwise_and(iota((seqs, all_slots), 1), cap - 1).astype(f32)
    right_rank = nt_dot(rank, tall) == wide_rank
    for k, one in enumerate(chosen):
        pick_v[k] = ((nt_dot(one, tall) > 0.5) & right_rank).astype(f32).astype(bf16)

    loads["mg"].wait()
    loads["win"].wait()
    for copy in gathers:
        copy.wait_recv()
    square = jnp.zeros((seqs, 1), f32)
    for t in range(n_tp):
        value = tok_v[t].astype(f32)
        square = square + jnp.sum(value * value, axis=1, keepdims=True)
    scale = lax.rsqrt(square * (1.0 / model) + epsilon)
    drive = jnp.zeros((seqs, channels), f32)
    for t in range(n_tp):
        columns = pl.ds(t * width, width)
        normed = (tok_v[t].astype(f32) * scale * mg_v[:, columns]).astype(bf16)
        drive = drive + nn_dot(normed, win_v[columns, :])
    drive = drive.astype(bf16)
    push = [nn_dot(drive, bt_v[i]) for i in range(2)]
    for piece in range(groups // pairs):
        lo = piece * 128
        at = pl.ds(lo, 128)
        f_re, f_im = rows_v[pl.ds(2, 1), at], rows_v[pl.ds(3, 1), at]
        x_re, x_im = push[0][:, lo : lo + 128], push[1][:, lo : lo + 128]
        new = (
            base_v[0, :, at] + (f_re * x_re - f_im * x_im),
            base_v[1, :, at] + (f_re * x_im + f_im * x_re),
        )
        for i in range(2):
            half_v[i, :, at] = new[i].astype(bf16)
            base_v[i, :, at] = new[i]
    readout = nt_dot(half_v[0], ct_v[0]) - nt_dot(half_v[1], ct_v[1])
    loads["skip"].wait()
    mixed = jax.nn.gelu(readout + skip_v[...] * drive.astype(f32)).astype(bf16)

    loads["wo"].wait()
    scatters = []
    for d in range(1, n_tp):
        columns = pl.ds(pl.multiple_of(tp_to(d) * width, 128), width)
        part_v[d - 1] = nn_dot(mixed, wo_v[:, columns]).astype(bf16)
        copy = remote(
            part_v.at[d - 1], part_in.at[d - 1], rs_s.at[d - 1], rs_r.at[d - 1], {"tp": tp_to(d)}
        )
        copy.start()
        scatters.append(copy)
    columns = pl.ds(pl.multiple_of(me_t * width, 128), width)
    total = nn_dot(mixed, wo_v[:, columns]) + tok_v[me_t].astype(f32)
    for piece in range(groups // pairs):
        for i in range(2):
            for k in range(pairs):
                ns_v[i, pl.ds(piece * pairs + k, seqs, stride=groups), :] = base_v[
                    i, :, piece * 128 + k * states : piece * 128 + (k + 1) * states
                ]
    keep_state = pltpu.make_async_copy(ns_v, new_state, store_sem.at[0])
    keep_state.start()
    for d in range(1, n_tp):
        scatters[d - 1].wait_recv()
        total = total + part_in[d - 1].astype(f32)
    resid = total.astype(bf16)
    resid_v[...] = resid

    slot_rows = nn_dot(sel_v[...], resid).astype(bf16)
    slot_v[...] = slot_rows.reshape(n_ep, local_e, cap, width)
    dispatches = {}
    for j in range(local_e):
        for d in range(1, n_ep):
            sem = j * (n_ep - 1) + d - 1
            copy = remote(
                slot_v.at[ep_to(d), j], x_v.at[j, me_t, me_e], dp_s.at[sem], dp_r.at[sem],
                {"ep": ep_to(d)},
            )
            copy.start()
            dispatches[j, d] = copy
    for j in range(local_e):
        x_v[j, me_t, me_e] = slot_v[me_e, j]
    beside = (me_t + 1 - 2 * lax.rem(me_t, 2), lax.rem(me_t + 2, n_tp))
    forwards = {}

    def forward(j, d):
        if d:
            dispatches[j, d].wait_recv()
        block = x_v.at[j, me_t, ep_from(d)]
        for k in range(2):
            sem = (j * n_ep + d) * 3 + k
            copy = remote(block, block, fw_s.at[sem], fw_r.at[sem], {"tp": beside[k]})
            copy.start()
            forwards[j, d, k] = copy

    def hand_on(j, d):
        k = d % 2
        forwards[j, d, k].wait_recv()
        block = x_v.at[j, beside[k], ep_from(d)]
        sem = (j * n_ep + d) * 3 + 2
        copy = remote(block, block, fw_s.at[sem], fw_r.at[sem], {"tp": beside[1 - k]})
        copy.start()
        forwards[j, d, 2] = copy

    for d in range(n_ep):
        forward(0, d)
    for d in range(n_ep):
        hand_on(0, d)
    for j in range(1, local_e):
        for d in range(n_ep):
            forward(j, d)

    loads["fg"].wait()
    rows = n_ep * cap
    out_copies = []
    for j in range(local_e):
        for d in range(n_ep):
            forwards[j, d, 1 - d % 2].wait_recv()
            forwards[j, d, 2].wait_recv()
        blocks = [x_v[j, t].reshape(rows, width) for t in range(n_tp)]
        square = jnp.zeros((rows, 1), f32)
        for value in blocks:
            value = value.astype(f32)
            square = square + jnp.sum(value * value, axis=1, keepdims=True)
        scale = lax.rsqrt(square * (1.0 / model) + epsilon)
        for t in range(n_tp):
            columns = pl.ds(t * width, width)
            xn_v[:, columns] = (blocks[t].astype(f32) * scale * fg_v[:, columns]).astype(bf16)
        loads[("g", j)].wait()
        loads[("u", j)].wait()
        tile = 256

        @pl.loop(0, hidden // tile)
        def _(n, j=j):
            at = pl.ds(pl.multiple_of(n * tile, tile), tile)
            gate = nn_dot(xn_v[...], wg_v[j, :, at])
            up = nn_dot(xn_v[...], wu_v[j, :, at])
            hid_v[:, at] = (jax.nn.silu(gate) * up).astype(bf16)

        if j + 1 < local_e:
            for d in range(n_ep // 2):
                hand_on(j + 1, d)
        loads[("d", j)].wait()
        for d in range(1, n_tp):
            columns = pl.ds(pl.multiple_of(tp_to(d) * width, 128), width)
            at = j * (n_tp - 1) + d - 1
            oo_v[at] = nn_dot(hid_v[...], wd_v[j, :, columns]).astype(bf16)
            copy = remote(oo_v.at[at], oo_in.at[at], os_s.at[at], os_r.at[at], {"tp": tp_to(d)})
            copy.start()
            out_copies.append(copy)
        columns = pl.ds(pl.multiple_of(me_t * width, 128), width)
        own_v[j] = nn_dot(hid_v[...], wd_v[j, :, columns])
        if j + 1 < local_e:
            for d in range(n_ep // 2, n_ep):
                hand_on(j + 1, d)

    returns = []
    for j in range(local_e):
        total = own_v[j]
        for d in range(1, n_tp):
            at = j * (n_tp - 1) + d - 1
            out_copies[at].wait_recv()
            total = total + oo_in[at].astype(f32)
        ro_v[j] = total.astype(bf16).reshape(n_ep, cap, width)
        for d in range(1, n_ep):
            at = j * (n_ep - 1) + d - 1
            copy = remote(
                ro_v.at[j, ep_to(d)], ret_v.at[me_e, j], rt_s.at[at], rt_r.at[at],
                {"ep": ep_to(d)},
            )
            copy.start()
            returns.append(copy)
        ret_v[me_e, j] = ro_v[j, me_e]
    loads["rw"].wait()
    for copy in returns:
        copy.wait_recv()
    result = resid_v[...].astype(f32)
    back = ret_v[...].reshape(all_slots, width)
    for k in range(len(chosen)):
        result = result + to_column(rw_v[k : k + 1, :]) * nn_dot(pick_v[k], back)
    out_v[...] = result.astype(bf16)
    keep_out = pltpu.make_async_copy(out_v, out, store_sem.at[1])
    keep_out.start()
    for copy in gathers + scatters + list(dispatches.values()) + list(
        forwards.values()
    ) + out_copies + returns:
        copy.wait_send()
    keep_state.wait()
    keep_out.wait()


def fused(
    tokens, mix_gain, w_in, a_real, a_imag, log_step, b_coef, output_coefficients, skip, w_out,
    state, ffn_gain, w_gate, w_up, w_down, expert_ids, route_weights,
):
    bf16, f32 = jnp.bfloat16, jnp.float32
    n_tp, n_ep = lax.axis_size("tp"), lax.axis_size("ep")
    seqs, width = tokens.shape
    groups, states = a_real.shape
    chans = b_coef.shape[3]
    local_e, model, hidden = w_gate.shape
    top = expert_ids.shape[1]
    experts = local_e * n_ep
    cap = max(2, 2 * seqs * top // experts)
    lanes, channels = groups * states, groups * chans
    rows = n_ep * cap
    sizes = (n_tp, n_ep, seqs, width, groups, states, chans, cap, local_e, hidden)
    args = (
        tokens, mix_gain[None], w_in, a_real, a_imag, log_step[None],
        b_coef.transpose(0, 1, 3, 2).reshape(2, channels, states), output_coefficients.reshape(2, channels, states),
        skip[None], w_out, state.reshape(2, seqs * groups, states), ffn_gain[None],
        w_gate, w_up, w_down, expert_ids.T, route_weights.T,
    )
    vmem = pltpu.VMEM
    scratch = [vmem((n_tp, seqs, width), bf16)]
    scratch += [vmem(a.shape, a.dtype) for a in args[1:]]
    scratch += [
        vmem((2, channels, lanes), bf16),
        vmem((2, channels, lanes), bf16),
        vmem((8, lanes), f32),
        vmem((2, seqs, lanes), f32),
        vmem((2, seqs * groups, states), f32),
        vmem((2, seqs, lanes), bf16),
        vmem((n_tp - 1, seqs, width), bf16),
        vmem((n_tp - 1, seqs, width), bf16),
        vmem((experts * cap, seqs), bf16),
        vmem((top, seqs, experts * cap), bf16),
        vmem((seqs, width), bf16),
        vmem((n_ep, local_e, cap, width), bf16),
        vmem((local_e, n_tp, n_ep, cap, width), bf16),
        vmem((rows, model), bf16),
        vmem((rows, hidden), bf16),
        vmem((local_e * (n_tp - 1), rows, width), bf16),
        vmem((local_e, rows, width), f32),
        vmem((local_e * (n_tp - 1), rows, width), bf16),
        vmem((local_e, n_ep, cap, width), bf16),
        vmem((n_ep, local_e, cap, width), bf16),
        vmem((seqs, width), bf16),
    ]
    dma = pltpu.SemaphoreType.DMA
    counts = [14, 3 * local_e, 2]
    for number in (
        n_tp - 1, n_tp - 1, local_e * (n_ep - 1), local_e * n_ep * 3, local_e * (n_tp - 1),
        local_e * (n_ep - 1),
    ):
        counts += [number, number]
    scratch += [dma((number,)) for number in counts]
    out, new_state = pl.pallas_call(
        functools.partial(fused_body, sizes),
        out_shape=(
            jax.ShapeDtypeStruct((seqs, width), bf16),
            jax.ShapeDtypeStruct((2, seqs * groups, states), f32),
        ),
        in_specs=[pl.BlockSpec(memory_space=HBM)] * len(args),
        out_specs=(pl.BlockSpec(memory_space=HBM),) * 2,
        scratch_shapes=scratch,
        compiler_params=pltpu.CompilerParams(
            collective_id=0, has_side_effects=True, vmem_limit_bytes=60 * 1024 * 1024
        ),
    )(*args)
    out, new_state = hand_over(out, new_state)
    return out, new_state.reshape(state.shape)


def hand_over_body(out, new_state, out_to, state_to, out_v, state_v, sems):
    pieces = [(out, out_v, out_to)]
    part = new_state.shape[1] // 2
    for i in range(2):
        for k in range(2):
            at = (i, pl.ds(k * part, part))
            pieces.append((new_state.at[at], state_v.at[at], state_to.at[at]))
    reads = [
        pltpu.make_async_copy(src, mid, sems.at[0, n]) for n, (src, mid, _) in enumerate(pieces)
    ]
    writes = [
        pltpu.make_async_copy(mid, dst, sems.at[1, n]) for n, (_, mid, dst) in enumerate(pieces)
    ]
    for copy in reads:
        copy.start()
    for read, write in zip(reads, writes):
        read.wait()
        write.start()
    for copy in writes:
        copy.wait()


def hand_over(out, new_state):
    return pl.pallas_call(
        hand_over_body,
        out_shape=tuple(jax.ShapeDtypeStruct(a.shape, a.dtype) for a in (out, new_state)),
        in_specs=[pl.BlockSpec(memory_space=HBM)] * 2,
        out_specs=(pl.BlockSpec(memory_space=HBM),) * 2,
        scratch_shapes=[
            pltpu.VMEM(out.shape, out.dtype),
            pltpu.VMEM(new_state.shape, new_state.dtype),
            pltpu.SemaphoreType.DMA((2, 5)),
        ],
    )(out, new_state)


def fits(mesh_tp, width, groups, states, chans, cap, hidden):
    powers = all(v & (v - 1) == 0 for v in (states, chans, cap))
    return (
        powers and mesh_tp == 4 and width % 128 == 0 and states <= 128 and groups % max(8, 128 // states) == 0
        and cap % 16 == 0 and (groups * chans) % 128 == 0 and hidden % 256 == 0
    )


def layer(*args):
    tokens, a_real, b_coef, w_gate, ids = args[0], args[3], args[6], args[12], args[15]
    experts = w_gate.shape[0] * lax.axis_size("ep")
    cap = max(2, 2 * tokens.shape[0] * ids.shape[1] // experts)
    kernel = fits(
        lax.axis_size("tp"), tokens.shape[1], *a_real.shape, b_coef.shape[3], cap, w_gate.shape[2]
    )
    return fused(*args) if kernel else local(*args)


def solution(mesh):
    in_specs = (
        P("ep", "tp"),
        P(),
        P(None, "tp"),
        P("tp", None),
        P("tp", None),
        P("tp"),
        P(None, "tp", None, None),
        P(None, "tp", None, None),
        P("tp"),
        P("tp", None),
        P(None, "ep", "tp", None),
        P(),
        P("ep", None, "tp"),
        P("ep", None, "tp"),
        P("ep", "tp", None),
        P("ep", None),
        P("ep", None),
    )
    out_specs = (P("ep", "tp"), P(None, "ep", "tp", None))
    return jax.shard_map(layer, mesh=mesh, in_specs=in_specs, out_specs=out_specs, check_vma=False)
```
